32 devices in a mesh: kv: 4 (over y, x), tp: 8 (over z, core).
Axes of the slice: x: 2, y: 2, z: 4, core: 2. Of those that a mesh axis runs over, the one named last changes fastest.
Arguments:
- residual: bfloat16 [128, 4096], P(None, ('kv', 'tp')), may hold values from -20 to 20
- mixer_gain: float32 [4096], P('kv'), may hold values from 0.1 to 1.9
- w_query: bfloat16 [4096, 4096], P('kv', 'tp'), may hold values from -0.09375 to 0.09375
- w_forget: bfloat16 [4096, 4096], P('kv', 'tp'), may hold values from -0.09375 to 0.09375
- w_input: bfloat16 [4096, 4096], P('kv', 'tp'), may hold values from -0.09375 to 0.09375
- w_outgate: bfloat16 [4096, 4096], P('kv', 'tp'), may hold values from -0.09375 to 0.09375
- lower_bound: float32 [4096], P('tp'), may hold values from 0.3 to 0.97
- state: float32 [128, 32, 128, 128], P('kv', 'tp'), may hold values from -6 to 6
- head_gain: float32 [128], replicated, may hold values from 0.1 to 1.9
- w_mix_out: bfloat16 [4096, 4096], P('tp', 'kv'), may hold values from -0.09375 to 0.09375
- ffn_gain: float32 [4096], P('kv'), may hold values from 0.1 to 1.9
- w_gate: bfloat16 [4096, 10752], P('kv', 'tp'), may hold values from -0.09375 to 0.09375
- w_up: bfloat16 [4096, 10752], P('kv', 'tp'), may hold values from -0.09375 to 0.09375
- w_down: bfloat16 [10752, 4096], P('tp', 'kv'), may hold values from -0.0625 to 0.0625
Outputs:
- layer_out: bfloat16 [128, 4096], P(None, ('kv', 'tp'))
- new_state: float32 [128, 32, 128, 128], P('kv', 'tp')
The draws below stay inside these ranges and needn't reach their ends.
All inputs are finite; a program needn't handle non-finite values.
Results may differ from the reference program's by a relative error of at most 0.015.
Values may be sent and summed in bfloat16 or wider, within the bound.
A program may use at most 64 MiB of HBM per device.

```python
import jax
import jax.numpy as jnp
from jax import lax

D = 4096
HEADS = 32
DK = 128
DV = 128
FF = 10752
SEQS = 128
HID = 4096
VID = 4096
N_KV = 4
N_TP = 8


def draw_residual(key, part):
    first = jax.random.fold_in(jax.random.fold_in(key, 11), 0)
    column = jnp.arange(D)
    kv_index = (column // (D // N_KV)).astype(jnp.float32)
    tp_index = (column // (D // (N_KV * N_TP)) % N_TP).astype(jnp.float32)
    col_scale = 0.4 * 3.0 ** (kv_index / max(N_KV - 1, 1)) * 3.0 ** (tp_index / max(N_TP - 1, 1))
    values = jnp.clip(jax.random.normal(first, (SEQS, D), jnp.float32), -4.0, 4.0)
    return jnp.clip(values * col_scale, -20.0, 20.0).astype(jnp.bfloat16)


def block_scale(stream_key, extent, pieces, smallest, high):
    gain = 1.0
    for position, shards_of in pieces:
        heights = jax.random.uniform(jax.random.fold_in(jax.random.fold_in(stream_key, 6), position), (shards_of,), jnp.float32, smallest / len(pieces), high / len(pieces))
        gain = gain * jnp.repeat(jnp.exp(heights), extent[position] // shards_of).reshape((-1,) + (1,) * (len(extent) - 1 - position))
    return gain


def scatter_about(stream_key, dims, scale, most, cuts=(), held_as=jnp.bfloat16):
    drawn = scale * jax.random.normal(stream_key, dims, jnp.float32)
    if cuts:
        drawn = drawn * block_scale(stream_key, dims, cuts, -0.22, 0.18)
    return jnp.clip(drawn, -most, most).astype(held_as)


def setup_inputs(seed: int = 0) -> dict:
    key_of = jax.random.split(jax.random.key(seed), 15)
    return {
        "residual": draw_residual(jax.random.fold_in(key_of[14], 71), 0),
        "mixer_gain": jnp.clip(1.0 + 0.18 * jax.random.normal(key_of[1], (D,), jnp.float32), 0.1, 1.9),
        "w_query": scatter_about(key_of[2], (D, HID), D ** -0.5, 0.09375, ((0, 4), (1, 8))),
        "w_forget": scatter_about(key_of[3], (D, HID), D ** -0.5, 0.09375, ((0, 4), (1, 8))),
        "w_input": scatter_about(key_of[4], (D, VID), D ** -0.5, 0.09375, ((0, 4), (1, 8))),
        "w_outgate": scatter_about(key_of[5], (D, VID), D ** -0.5, 0.09375, ((0, 4), (1, 8))),
        "lower_bound": jnp.clip(0.3 + 0.67 * jax.random.uniform(key_of[6], (HID,), jnp.float32) ** block_scale(key_of[6], (HID,), ((0, 8),), -0.2, 0.2), 0.3, 0.97),
        "state": scatter_about(key_of[7], (SEQS, HEADS, DK, DV), 1.0, 6.0, ((0, 4), (1, 8)), jnp.float32),
        "head_gain": jnp.clip(1.0 + 0.18 * jax.random.normal(key_of[8], (DV,), jnp.float32), 0.1, 1.9),
        "w_mix_out": scatter_about(key_of[9], (VID, D), VID ** -0.5, 0.09375, ((0, 8), (1, 4))),
        "ffn_gain": jnp.clip(1.0 + 0.18 * jax.random.normal(key_of[10], (D,), jnp.float32), 0.1, 1.9),
        "w_gate": scatter_about(key_of[11], (D, FF), D ** -0.5, 0.09375, ((0, 4), (1, 8))),
        "w_up": scatter_about(key_of[12], (D, FF), D ** -0.5, 0.09375, ((0, 4), (1, 8))),
        "w_down": scatter_about(key_of[13], (FF, D), FF ** -0.5, 0.0625, ((0, 8), (1, 4))),
    }


EPS = 1e-06

def reference(residual, mixer_gain, w_query, w_forget, w_input, w_outgate, lower_bound, state, head_gain, w_mix_out, ffn_gain, w_gate, w_up, w_down):
    seqs = residual.shape[0]
    xf = residual.astype(jnp.float32)
    inv_a = lax.rsqrt(lax.optimization_barrier(jnp.mean(xf * xf, axis=1, keepdims=True)) + EPS)
    scaled_a = (xf * mixer_gain).astype(jnp.bfloat16)
    query_raw = inv_a * jnp.dot(scaled_a, w_query, preferred_element_type=jnp.float32)
    forget_raw = inv_a * jnp.dot(scaled_a, w_forget, preferred_element_type=jnp.float32)
    value_raw = inv_a * jnp.dot(scaled_a, w_input, preferred_element_type=jnp.float32)
    outgate_raw = inv_a * jnp.dot(scaled_a, w_outgate, preferred_element_type=jnp.float32)
    bound = lower_bound.reshape(HEADS, DK)
    forget_raw = forget_raw.reshape(seqs, HEADS, DK)
    forget = bound + (1.0 - bound) * jax.nn.sigmoid(forget_raw)
    keyvec = (1.0 - bound) * jax.nn.sigmoid(-forget_raw)
    query = jax.nn.silu(query_raw.reshape(seqs, HEADS, DK))
    values = value_raw.reshape(seqs, HEADS, DV)
    new_state = forget[..., None] * state + keyvec[..., None] * values[:, :, None, :]
    head_out = jnp.einsum('shc,shce->she', query, new_state, precision=lax.Precision.HIGHEST)
    inv_h = lax.rsqrt(lax.optimization_barrier(jnp.mean(head_out * head_out, axis=2, keepdims=True)) + EPS)
    normed = head_out * inv_h * head_gain * jax.nn.silu(outgate_raw.reshape(seqs, HEADS, DV))
    normed = normed.reshape(seqs, HEADS * DV).astype(jnp.bfloat16)
    after_mix = (xf + jnp.dot(normed, w_mix_out, preferred_element_type=jnp.float32)).astype(jnp.bfloat16)
    af = after_mix.astype(jnp.float32)
    inv_b = lax.rsqrt(lax.optimization_barrier(jnp.mean(af * af, axis=1, keepdims=True)) + EPS)
    scaled_b = (af * ffn_gain).astype(jnp.bfloat16)
    gate = inv_b * jnp.dot(scaled_b, w_gate, preferred_element_type=jnp.float32)
    upper = inv_b * jnp.dot(scaled_b, w_up, preferred_element_type=jnp.float32)
    hidden = (jax.nn.silu(gate) * upper).astype(jnp.bfloat16)
    layer_out = (af + jnp.dot(hidden, w_down, preferred_element_type=jnp.float32)).astype(jnp.bfloat16)
    return (layer_out, new_state)
```

```python
import functools

import jax
import jax.numpy as jnp
from jax import lax
from jax.experimental import pallas as pl
from jax.experimental.pallas import tpu as pltpu
from jax.sharding import PartitionSpec as P

EPS = 1e-06
F32 = jnp.float32
BF16 = jnp.bfloat16
LANES = 128


def ring(axis, size):
    me = lax.axis_index(axis)
    return me, [lax.rem(me + step, size) for step in range(1, size)]


def greet(axes):
    barrier = pltpu.get_barrier_semaphore()
    count = 0
    for axis, peers in axes:
        for peer in peers:
            pl.semaphore_signal(
                barrier, inc=1, device_id={axis: peer}, device_id_type=pl.DeviceIdType.MESH
            )
            count += 1
    pl.semaphore_wait(barrier, count)


def remote(source, target, send_sem, recv_sem, axis, peer):
    return pltpu.make_async_remote_copy(
        src_ref=source,
        dst_ref=target,
        send_sem=send_sem,
        recv_sem=recv_sem,
        device_id={axis: peer},
        device_id_type=pl.DeviceIdType.MESH,
    )


def scale_block(blocks, gain_ref, scaled, count, width):
    squares = None
    for j in range(count):
        rows = blocks[j].astype(F32)
        cols = slice(j * width, (j + 1) * width)
        scaled[:, cols] = (rows * gain_ref[:, cols]).astype(BF16)
        term = rows * rows
        squares = term if squares is None else squares + term
    total = jnp.sum(squares, axis=1, keepdims=True)
    return jnp.broadcast_to(total, (total.shape[0], LANES))


def project_kernel(
    n_kv, n_tp, features,
    x_ref, gain_ref, wq, wf, wi, wo,
    out_ref,
    weights, blocks, scaled, parts, landed, squares, squares_in,
    w_sem, x_send, x_recv, p_send, p_recv, s_send, s_recv,
):
    seqs, width = x_ref.shape
    local = out_ref.shape[1]
    loads = [
        pltpu.make_async_copy(source, weights.at[i], w_sem.at[i])
        for i, source in enumerate((wq, wf, wi, wo))
    ]
    for load in loads:
        load.start()
    kv, kv_peers = ring("kv", n_kv)
    tp, tp_peers = ring("tp", n_tp)
    greet((("kv", kv_peers), ("tp", tp_peers)))

    gathers = [
        remote(x_ref, blocks.at[tp], x_send.at[i], x_recv.at[i], "tp", peer)
        for i, peer in enumerate(tp_peers)
    ]
    for copy in gathers:
        copy.start()
    blocks[pl.ds(tp, 1)] = x_ref[...][None]
    for copy in gathers:
        copy.wait_recv()
    squares[...] = scale_block(blocks, gain_ref, scaled, n_tp, width)
    square_copies = [
        remote(
            squares.at[pl.ds(pl.multiple_of(peer * local, local), local), :],
            squares_in.at[i], s_send.at[i], s_recv.at[i], "kv", peer,
        )
        for i, peer in enumerate(kv_peers)
    ]
    for copy in square_copies:
        copy.start()
    for load in loads:
        load.wait()
    part_copies = []
    for p in range(4):
        parts[p] = jnp.dot(scaled[...], weights[p], preferred_element_type=F32).astype(BF16)
        for i, peer in enumerate(kv_peers):
            copy = remote(
                parts.at[p, pl.ds(pl.multiple_of(peer * local, local), local), :],
                landed.at[i, p], p_send.at[i, p], p_recv.at[i, p], "kv", peer,
            )
            copy.start()
            part_copies.append(copy)
    own = pl.ds(pl.multiple_of(kv * local, local), local)
    total = squares[own, :]
    for copy in square_copies:
        copy.wait_recv()
    for i in range(n_kv - 1):
        total = total + squares_in[i]
    inverse = lax.rsqrt(total[:, :1] / features + EPS)
    for copy in part_copies:
        copy.wait_recv()
    for p in range(4):
        value = parts[p, own, :].astype(F32)
        for i in range(n_kv - 1):
            value = value + landed[i, p].astype(F32)
        out_ref[p] = value * inverse
    for copy in gathers + square_copies + part_copies:
        copy.wait_send()


def state_kernel(q_ref, f_ref, v_ref, g_ref, bound_ref, gain_ref, state_ref, new_ref, normed_ref):
    rows = q_ref.shape[1]
    bound = bound_ref[...]
    raw = f_ref[0]
    forget = bound + (1.0 - bound) * jax.nn.sigmoid(raw)
    keyvec = (1.0 - bound) * jax.nn.sigmoid(-raw)
    query = q_ref[0] * jax.nn.sigmoid(q_ref[0])
    forget_t, keyvec_t, query_t = forget.T, keyvec.T, query.T
    for s in range(rows):
        new = (
            forget_t[:, s : s + 1] * state_ref[s, 0]
            + keyvec_t[:, s : s + 1] * v_ref[0, s : s + 1, :]
        )
        new_ref[s, 0] = new
        head = jnp.sum(query_t[:, s : s + 1] * new, axis=0, keepdims=True)
        inverse = lax.rsqrt(jnp.mean(head * head, axis=1, keepdims=True) + EPS)
        gate = g_ref[0, s : s + 1, :]
        normed_ref[s : s + 1, :] = head * inverse * gain_ref[...] * (gate * jax.nn.sigmoid(gate))


def mix_kernel(
    n_kv, n_tp, features,
    normed_ref, x_ref, gain_ref, w_mix, w_gate, w_up, w_down,
    out_ref,
    mix_w, gate_w, down_w, normed16, heads, terms, terms_in, mixed, blocks, scaled,
    squares, squares_in, parts, landed, hidden, hiddens, downs, downs_in,
    w_sem, n_send, n_recv, t_send, t_recv, m_send, m_recv, s_send, s_recv,
    g_send, g_recv, h_send, h_recv, d_send, d_recv,
):
    seqs, width = x_ref.shape
    local = normed_ref.shape[0]
    units = gate_w.shape[1]
    loads = [
        pltpu.make_async_copy(source, target, w_sem.at[i])
        for i, (source, target) in enumerate(
            ((w_mix, mix_w), (w_gate, gate_w.at[0]), (w_up, gate_w.at[1]), (w_down, down_w))
        )
    ]
    for load in loads:
        load.start()
    normed16[...] = normed_ref[...].astype(BF16)
    kv, kv_peers = ring("kv", n_kv)
    tp, tp_peers = ring("tp", n_tp)
    own = pl.ds(pl.multiple_of(kv * local, local), local)
    greet((("kv", kv_peers), ("tp", tp_peers)))

    pending = []
    copies = [
        remote(normed16, heads.at[own, :], n_send.at[i], n_recv.at[i], "kv", peer)
        for i, peer in enumerate(kv_peers)
    ]
    for copy in copies:
        copy.start()
    pending += copies
    heads[own, :] = normed16[...]
    loads[0].wait()
    for copy in copies:
        copy.wait_recv()

    group = max(1, 256 // width)
    while n_tp % group:
        group -= 1

    def scatter(left, weight, sums, sums_in, send, recv):
        for t in range(0, n_tp, group):
            part = jnp.dot(
                left[...], weight[:, t * width : (t + group) * width], preferred_element_type=F32
            ).astype(BF16)
            for j in range(group):
                sums[t + j] = part[:, j * width : (j + 1) * width]
        out = [
            remote(sums.at[peer], sums_in.at[i], send.at[i], recv.at[i], "tp", peer)
            for i, peer in enumerate(tp_peers)
        ]
        for copy in out:
            copy.start()
        return out

    def collect(base, sums, sums_in, out):
        total = base + sums[pl.ds(tp, 1)][0].astype(F32)
        for copy in out:
            copy.wait_recv()
        for i in range(n_tp - 1):
            total = total + sums_in[i].astype(F32)
        return total.astype(BF16)

    copies = scatter(heads, mix_w, terms, terms_in, t_send, t_recv)
    pending += copies
    mixed[...] = collect(x_ref[...].astype(F32), terms, terms_in, copies)

    copies = [
        remote(mixed, blocks.at[tp], m_send.at[i], m_recv.at[i], "tp", peer)
        for i, peer in enumerate(tp_peers)
    ]
    for copy in copies:
        copy.start()
    pending += copies
    blocks[pl.ds(tp, 1)] = mixed[...][None]
    for copy in copies:
        copy.wait_recv()
    squares[...] = scale_block(blocks, gain_ref, scaled, n_tp, width)
    square_copies = [
        remote(
            squares.at[pl.ds(pl.multiple_of(peer * local, local), local), :],
            squares_in.at[i], s_send.at[i], s_recv.at[i], "kv", peer,
        )
        for i, peer in enumerate(kv_peers)
    ]
    for copy in square_copies:
        copy.start()
    pending += square_copies

    copies = []
    step = min(512, units)
    for g in range(2):
        loads[1 + g].wait()
        for c in range(0, units, step):
            end = min(c + step, units)
            parts[g, :, c:end] = lax.dot_general(
                scaled[...], gate_w[g, c:end, :], (((1,), (1,)), ((), ())),
                preferred_element_type=F32,
            ).astype(BF16)
        for i, peer in enumerate(kv_peers):
            copy = remote(
                parts.at[g, pl.ds(pl.multiple_of(peer * local, local), local), :],
                landed.at[i, g], g_send.at[i, g], g_recv.at[i, g], "kv", peer,
            )
            copy.start()
            copies.append(copy)
    pending += copies
    for copy in square_copies:
        copy.wait_recv()
    total = squares[own, :]
    for i in range(n_kv - 1):
        total = total + squares_in[i]
    inverse = lax.rsqrt(total[:, :1] / features + EPS)
    for copy in copies:
        copy.wait_recv()
    sums = []
    for g in range(2):
        value = parts[g, own, :].astype(F32)
        for i in range(n_kv - 1):
            value = value + landed[i, g].astype(F32)
        sums.append(value * inverse)
    hidden[...] = (sums[0] * jax.nn.sigmoid(sums[0]) * sums[1]).astype(BF16)

    copies = [
        remote(hidden, hiddens.at[own, :], h_send.at[i], h_recv.at[i], "kv", peer)
        for i, peer in enumerate(kv_peers)
    ]
    for copy in copies:
        copy.start()
    pending += copies
    hiddens[own, :] = hidden[...]
    loads[3].wait()
    for copy in copies:
        copy.wait_recv()
    copies = scatter(hiddens, down_w, downs, downs_in, d_send, d_recv)
    pending += copies
    out_ref[...] = collect(mixed[...].astype(F32), downs, downs_in, copies)
    for copy in pending:
        copy.wait_send()


def in_vmem():
    return pl.BlockSpec(memory_space=pltpu.VMEM)


def in_hbm():
    return pl.BlockSpec(memory_space=pl.ANY)


def body(
    n_kv, n_tp,
    residual, mixer_gain, w_query, w_forget, w_input, w_outgate, lower_bound, state,
    head_gain, w_mix_out, ffn_gain, w_gate, w_up, w_down,
):
    seqs, width = residual.shape
    depth, hid = w_query.shape
    local, heads, dk, dv = state.shape
    units = w_gate.shape[1]
    features = depth * n_kv
    dma = pltpu.SemaphoreType.DMA

    raw = pl.pallas_call(
        functools.partial(project_kernel, n_kv, n_tp, features),
        out_shape=jax.ShapeDtypeStruct((4, local, hid), F32),
        in_specs=[in_vmem()] * 2 + [in_hbm()] * 4,
        out_specs=in_vmem(),
        scratch_shapes=[
            pltpu.VMEM((4, depth, hid), BF16),
            pltpu.VMEM((n_tp, seqs, width), BF16),
            pltpu.VMEM((seqs, depth), BF16),
            pltpu.VMEM((4, seqs, hid), BF16),
            pltpu.VMEM((n_kv - 1, 4, local, hid), BF16),
            pltpu.VMEM((seqs, LANES), F32),
            pltpu.VMEM((n_kv - 1, local, LANES), F32),
            dma((4,)),
            dma((n_tp - 1,)), dma((n_tp - 1,)),
            dma((n_kv - 1, 4)), dma((n_kv - 1, 4)),
            dma((n_kv - 1,)), dma((n_kv - 1,)),
        ],
        compiler_params=pltpu.CompilerParams(collective_id=0, has_side_effects=True),
        name="project",
    )(residual, mixer_gain.reshape(1, depth), w_query, w_forget, w_input, w_outgate)

    rows = 16 if local % 16 == 0 else local
    pick = lambda p: pl.BlockSpec((1, rows, dk), lambda h, s: (p, s, h))
    updated, normed = pl.pallas_call(
        state_kernel,
        grid=(heads, local // rows),
        out_shape=(
            jax.ShapeDtypeStruct(state.shape, F32),
            jax.ShapeDtypeStruct((local, heads * dv), F32),
        ),
        in_specs=[
            pick(0), pick(1), pick(2), pick(3),
            pl.BlockSpec((1, dk), lambda h, s: (0, h)),
            pl.BlockSpec((1, dv), lambda h, s: (0, 0)),
            pl.BlockSpec((rows, 1, dk, dv), lambda h, s: (s, h, 0, 0)),
        ],
        out_specs=(
            pl.BlockSpec((rows, 1, dk, dv), lambda h, s: (s, h, 0, 0)),
            pl.BlockSpec((rows, dv), lambda h, s: (s, h)),
        ),
        name="state",
    )(raw, raw, raw, raw, lower_bound.reshape(1, hid), head_gain.reshape(1, dv), state)

    layer_out = pl.pallas_call(
        functools.partial(mix_kernel, n_kv, n_tp, features),
        out_shape=jax.ShapeDtypeStruct((seqs, width), BF16),
        in_specs=[in_vmem()] * 3 + [in_hbm()] * 4,
        out_specs=in_vmem(),
        scratch_shapes=[
            pltpu.VMEM(w_mix_out.shape, BF16),
            pltpu.VMEM((2, units, depth), BF16),
            pltpu.VMEM(w_down.shape, BF16),
            pltpu.VMEM((local, hid), BF16),
            pltpu.VMEM((seqs, hid), BF16),
            pltpu.VMEM((n_tp, seqs, width), BF16),
            pltpu.VMEM((n_tp - 1, seqs, width), BF16),
            pltpu.VMEM((seqs, width), BF16),
            pltpu.VMEM((n_tp, seqs, width), BF16),
            pltpu.VMEM((seqs, depth), BF16),
            pltpu.VMEM((seqs, LANES), F32),
            pltpu.VMEM((n_kv - 1, local, LANES), F32),
            pltpu.VMEM((2, seqs, units), BF16),
            pltpu.VMEM((n_kv - 1, 2, local, units), BF16),
            pltpu.VMEM((local, units), BF16),
            pltpu.VMEM((seqs, units), BF16),
            pltpu.VMEM((n_tp, seqs, width), BF16),
            pltpu.VMEM((n_tp - 1, seqs, width), BF16),
            dma((4,)),
            dma((n_kv - 1,)), dma((n_kv - 1,)),
            dma((n_tp - 1,)), dma((n_tp - 1,)),
            dma((n_tp - 1,)), dma((n_tp - 1,)),
            dma((n_kv - 1,)), dma((n_kv - 1,)),
            dma((n_kv - 1, 2)), dma((n_kv - 1, 2)),
            dma((n_kv - 1,)), dma((n_kv - 1,)),
            dma((n_tp - 1,)), dma((n_tp - 1,)),
        ],
        compiler_params=pltpu.CompilerParams(collective_id=1, has_side_effects=True),
        name="mix",
    )(normed, residual, ffn_gain.reshape(1, depth), w_mix_out, w_gate.T, w_up.T, w_down)
    return layer_out, updated


def solution(mesh):
    in_specs = (
        P(None, ("kv", "tp")),
        P("kv"),
        P("kv", "tp"),
        P("kv", "tp"),
        P("kv", "tp"),
        P("kv", "tp"),
        P("tp"),
        P("kv", "tp", None, None),
        P(),
        P("tp", "kv"),
        P("kv"),
        P("kv", "tp"),
        P("kv", "tp"),
        P("tp", "kv"),
    )
    out_specs = (P(None, ("kv", "tp")), P("kv", "tp", None, None))
    return jax.shard_map(
        functools.partial(body, mesh.shape["kv"], mesh.shape["tp"]),
        mesh=mesh, in_specs=in_specs, out_specs=out_specs, check_vma=False,
    )
```

```python
import functools

import jax
import jax.numpy as jnp
from jax import lax
from jax.experimental import pallas as pl
from jax.experimental.pallas import tpu as pltpu
from jax.sharding import PartitionSpec as P

EPS = 1e-06
F32 = jnp.float32
BF16 = jnp.bfloat16
LANES = 128


def ring(axis, size):
    me = lax.axis_index(axis)
    return me, [lax.rem(me + step, size) for step in range(1, size)]


def greet(axes):
    barrier = pltpu.get_barrier_semaphore()
    count = 0
    for axis, peers in axes:
        for peer in peers:
            pl.semaphore_signal(
                barrier, inc=1, device_id={axis: peer}, device_id_type=pl.DeviceIdType.MESH
            )
            count += 1
    pl.semaphore_wait(barrier, count)


def remote(source, target, send_sem, recv_sem, axis, peer):
    return pltpu.make_async_remote_copy(
        src_ref=source,
        dst_ref=target,
        send_sem=send_sem,
        recv_sem=recv_sem,
        device_id={axis: peer},
        device_id_type=pl.DeviceIdType.MESH,
    )


def pairs(n_tp):
    me = lax.axis_index("tp")
    core = lax.rem(me, 2)
    return me, core, lax.div(me, 2), me + 1 - 2 * core, n_tp // 2


def gather_pairs(n_tp, source, blocks, send, recv):
    me, _, _, partner, half = pairs(n_tp)
    peers = [lax.rem(me + 2 * i, n_tp) for i in range(1, half)]
    origins = [lax.rem(me - 2 * i + n_tp, n_tp) for i in range(1, half)]
    direct = [
        remote(source, blocks.at[me], send.at[i], recv.at[i], "tp", peer)
        for i, peer in enumerate(peers)
    ]
    direct.append(
        remote(source, blocks.at[me], send.at[half - 1], recv.at[half - 1], "tp", partner)
    )
    for copy in direct:
        copy.start()
    blocks[pl.ds(me, 1)] = source[...][None]
    relays = []
    for i, origin in enumerate(origins):
        direct[i].wait_recv()
        relay = remote(
            blocks.at[origin], blocks.at[origin],
            send.at[half + i], recv.at[half + i], "tp", partner,
        )
        relay.start()
        relays.append(relay)
    direct[-1].wait_recv()
    for relay in relays:
        relay.wait_recv()
    return direct + relays


def scale_block(blocks, gain_ref, scaled, count, width):
    squares = None
    for j in range(count):
        rows = blocks[j].astype(F32)
        cols = slice(j * width, (j + 1) * width)
        scaled[:, cols] = (rows * gain_ref[:, cols]).astype(BF16)
        term = rows * rows
        squares = term if squares is None else squares + term
    total = jnp.sum(squares, axis=1, keepdims=True)
    return jnp.broadcast_to(total, (total.shape[0], LANES))


def project_kernel(
    n_kv, n_tp, features,
    x_ref, gain_ref, wq, wf, wi, wo,
    out_ref,
    weights, blocks, scaled, parts, landed, squares, squares_in,
    w_sem, x_send, x_recv, p_send, p_recv, s_send, s_recv,
):
    seqs, width = x_ref.shape
    local = out_ref.shape[1]
    loads = [
        pltpu.make_async_copy(source, weights.at[i], w_sem.at[i])
        for i, source in enumerate((wq, wf, wi, wo))
    ]
    for load in loads:
        load.start()
    kv, kv_peers = ring("kv", n_kv)
    tp, tp_peers = ring("tp", n_tp)
    near = pairs(n_tp)[3]
    greet((("kv", kv_peers), ("tp", [near] + tp_peers[1::2])))

    gathers = gather_pairs(n_tp, x_ref, blocks, x_send, x_recv)
    squares[...] = scale_block(blocks, gain_ref, scaled, n_tp, width)
    square_copies = [
        remote(
            squares.at[pl.ds(pl.multiple_of(peer * local, local), local), :],
            squares_in.at[i], s_send.at[i], s_recv.at[i], "kv", peer,
        )
        for i, peer in enumerate(kv_peers)
    ]
    for copy in square_copies:
        copy.start()
    for load in loads:
        load.wait()
    part_copies = []
    for p in range(4):
        parts[p] = jnp.dot(scaled[...], weights[p], preferred_element_type=F32).astype(BF16)
        for i, peer in enumerate(kv_peers):
            copy = remote(
                parts.at[p, pl.ds(pl.multiple_of(peer * local, local), local), :],
                landed.at[i, p], p_send.at[i, p], p_recv.at[i, p], "kv", peer,
            )
            copy.start()
            part_copies.append(copy)
    own = pl.ds(pl.multiple_of(kv * local, local), local)
    total = squares[own, :]
    for copy in square_copies:
        copy.wait_recv()
    for i in range(n_kv - 1):
        total = total + squares_in[i]
    inverse = lax.rsqrt(total[:, :1] / features + EPS)
    for copy in part_copies:
        copy.wait_recv()
    for p in range(4):
        value = parts[p, own, :].astype(F32)
        for i in range(n_kv - 1):
            value = value + landed[i, p].astype(F32)
        out_ref[p] = value * inverse
    for copy in gathers + square_copies + part_copies:
        copy.wait_send()


def split(value):
    high = value.astype(BF16).astype(F32)
    return high, value - high


def state_kernel(q_ref, f_ref, v_ref, g_ref, bound_ref, gain_ref, state_ref, new_ref, normed_ref, heads):
    rows, width = q_ref.shape[1:]
    bound = bound_ref[...]
    raw = f_ref[0]
    forget = split(bound + (1.0 - bound) * jax.nn.sigmoid(raw))
    keyvec = split((1.0 - bound) * jax.nn.sigmoid(-raw))
    query = split(q_ref[0] * jax.nn.sigmoid(q_ref[0]))
    values = split(v_ref[0])
    left = jnp.concatenate([*forget, *keyvec, keyvec[0], *query], axis=0).T.astype(BF16)
    one, nil = jnp.ones((rows, width), F32), jnp.zeros((rows, width), F32)
    right = jnp.concatenate(
        [
            jnp.concatenate([one, one, nil, nil, nil, nil, nil], axis=0),
            jnp.concatenate([nil, nil, values[0], values[0], values[1], nil, nil], axis=0),
            jnp.concatenate([nil, nil, nil, nil, nil, one, one], axis=0),
        ],
        axis=1,
    ).astype(BF16)
    owner = lax.rem(lax.broadcasted_iota(jnp.int32, right.shape, 0), rows)
    for s in range(rows):
        mask = jnp.where(owner == s, 1.0, 0.0).astype(BF16)
        wide = jnp.dot(left, right * mask, preferred_element_type=F32)
        new = wide[:, :width] * state_ref[s, 0] + wide[:, width : 2 * width]
        new_ref[s, 0] = new
        heads[s : s + 1, :] = jnp.sum(wide[:, 2 * width :] * new, axis=0, keepdims=True)
    head = heads[...]
    inverse = lax.rsqrt(jnp.mean(head * head, axis=1, keepdims=True) + EPS)
    gate = g_ref[0]
    normed_ref[...] = head * inverse * gain_ref[...] * (gate * jax.nn.sigmoid(gate))


def mix_kernel(
    n_kv, n_tp, features,
    normed_ref, x_ref, gain_ref, w_mix, w_gate, w_up, w_down,
    out_ref,
    mix_w, gate_w, down_w, normed16, heads, terms, terms_pair, terms_out, terms_in, mixed, blocks, scaled,
    squares, squares_in, parts, landed, hidden, hiddens, downs, downs_pair, downs_out, downs_in,
    w_sem, n_send, n_recv, t_send, t_recv, m_send, m_recv, s_send, s_recv,
    g_send, g_recv, h_send, h_recv, d_send, d_recv,
):
    seqs, width = x_ref.shape
    local = normed_ref.shape[0]
    units = gate_w.shape[1]
    loads = [
        pltpu.make_async_copy(source, target, w_sem.at[i])
        for i, (source, target) in enumerate(
            ((w_mix, mix_w), (w_gate, gate_w.at[0]), (w_up, gate_w.at[1]), (w_down, down_w))
        )
    ]
    for load in loads:
        load.start()
    normed16[...] = normed_ref[...].astype(BF16)
    kv, kv_peers = ring("kv", n_kv)
    tp, tp_peers = ring("tp", n_tp)
    own = pl.ds(pl.multiple_of(kv * local, local), local)
    near = pairs(n_tp)[3]
    greet((("kv", kv_peers), ("tp", [near] + tp_peers[1::2])))

    pending = []
    copies = [
        remote(normed16, heads.at[own, :], n_send.at[i], n_recv.at[i], "kv", peer)
        for i, peer in enumerate(kv_peers)
    ]
    for copy in copies:
        copy.start()
    pending += copies
    heads[own, :] = normed16[...]
    loads[0].wait()
    for copy in copies:
        copy.wait_recv()

    group = max(1, 256 // width)
    while n_tp % group:
        group -= 1

    me, core, chip, partner, half = pairs(n_tp)

    def reduce_pairs(base, left, weight, sums, pair_in, joined, sums_in, send, recv):
        for t in range(0, n_tp, group):
            part = jnp.dot(
                left[...], weight[:, t * width : (t + group) * width], preferred_element_type=F32
            ).astype(BF16)
            for j in range(group):
                sums[(t + j) % 2, (t + j) // 2] = part[:, j * width : (j + 1) * width]
        first = remote(sums.at[1 - core], pair_in, send.at[0], recv.at[0], "tp", partner)
        first.start()
        first.wait_recv()

        def pair_sum(place):
            mine = sums[pl.ds(core, 1), pl.ds(place, 1)][0, 0].astype(F32)
            return mine + pair_in[pl.ds(place, 1)][0].astype(F32)

        out = [first]
        for i in range(1, half):
            joined[i - 1] = pair_sum(lax.rem(chip + i, half)).astype(BF16)
            copy = remote(
                joined.at[i - 1], sums_in.at[i - 1], send.at[i], recv.at[i],
                "tp", lax.rem(me + 2 * i, n_tp),
            )
            copy.start()
            out.append(copy)
        total = base + pair_sum(chip)
        for i in range(1, half):
            out[i].wait_recv()
            total = total + sums_in[i - 1].astype(F32)
        pending.extend(out)
        return total.astype(BF16)

    mixed[...] = reduce_pairs(
        x_ref[...].astype(F32), heads, mix_w, terms, terms_pair, terms_out, terms_in, t_send, t_recv
    )

    pending += gather_pairs(n_tp, mixed, blocks, m_send, m_recv)
    squares[...] = scale_block(blocks, gain_ref, scaled, n_tp, width)
    square_copies = [
        remote(
            squares.at[pl.ds(pl.multiple_of(peer * local, local), local), :],
            squares_in.at[i], s_send.at[i], s_recv.at[i], "kv", peer,
        )
        for i, peer in enumerate(kv_peers)
    ]
    for copy in square_copies:
        copy.start()
    pending += square_copies

    copies = []
    step = min(512, units)
    for g in range(2):
        loads[1 + g].wait()
        for c in range(0, units, step):
            end = min(c + step, units)
            parts[g, :, c:end] = lax.dot_general(
                scaled[...], gate_w[g, c:end, :], (((1,), (1,)), ((), ())),
                preferred_element_type=F32,
            ).astype(BF16)
        for i, peer in enumerate(kv_peers):
            copy = remote(
                parts.at[g, pl.ds(pl.multiple_of(peer * local, local), local), :],
                landed.at[i, g], g_send.at[i, g], g_recv.at[i, g], "kv", peer,
            )
            copy.start()
            copies.append(copy)
    pending += copies
    for copy in square_copies:
        copy.wait_recv()
    total = squares[own, :]
    for i in range(n_kv - 1):
        total = total + squares_in[i]
    inverse = lax.rsqrt(total[:, :1] / features + EPS)
    for copy in copies:
        copy.wait_recv()
    sums = []
    for g in range(2):
        value = parts[g, own, :].astype(F32)
        for i in range(n_kv - 1):
            value = value + landed[i, g].astype(F32)
        sums.append(value * inverse)
    hidden[...] = (sums[0] * jax.nn.sigmoid(sums[0]) * sums[1]).astype(BF16)

    copies = [
        remote(hidden, hiddens.at[own, :], h_send.at[i], h_recv.at[i], "kv", peer)
        for i, peer in enumerate(kv_peers)
    ]
    for copy in copies:
        copy.start()
    pending += copies
    hiddens[own, :] = hidden[...]
    loads[3].wait()
    for copy in copies:
        copy.wait_recv()
    out_ref[...] = reduce_pairs(
        mixed[...].astype(F32), hiddens, down_w, downs, downs_pair, downs_out, downs_in, d_send, d_recv
    )
    for copy in pending:
        copy.wait_send()


def in_vmem():
    return pl.BlockSpec(memory_space=pltpu.VMEM)


def in_hbm():
    return pl.BlockSpec(memory_space=pl.ANY)


def body(
    n_kv, n_tp,
    residual, mixer_gain, w_query, w_forget, w_input, w_outgate, lower_bound, state,
    head_gain, w_mix_out, ffn_gain, w_gate, w_up, w_down,
):
    seqs, width = residual.shape
    depth, hid = w_query.shape
    local, heads, dk, dv = state.shape
    units = w_gate.shape[1]
    features = depth * n_kv
    half = n_tp // 2
    dma = pltpu.SemaphoreType.DMA

    raw = pl.pallas_call(
        functools.partial(project_kernel, n_kv, n_tp, features),
        out_shape=jax.ShapeDtypeStruct((4, local, hid), F32),
        in_specs=[in_vmem()] * 2 + [in_hbm()] * 4,
        out_specs=in_vmem(),
        scratch_shapes=[
            pltpu.VMEM((4, depth, hid), BF16),
            pltpu.VMEM((n_tp, seqs, width), BF16),
            pltpu.VMEM((seqs, depth), BF16),
            pltpu.VMEM((4, seqs, hid), BF16),
            pltpu.VMEM((n_kv - 1, 4, local, hid), BF16),
            pltpu.VMEM((seqs, LANES), F32),
            pltpu.VMEM((n_kv - 1, local, LANES), F32),
            dma((4,)),
            dma((n_tp - 1,)), dma((n_tp - 1,)),
            dma((n_kv - 1, 4)), dma((n_kv - 1, 4)),
            dma((n_kv - 1,)), dma((n_kv - 1,)),
        ],
        compiler_params=pltpu.CompilerParams(collective_id=0, has_side_effects=True),
        name="project",
    )(residual, mixer_gain.reshape(1, depth), w_query, w_forget, w_input, w_outgate)

    rows = 16 if local % 16 == 0 else local
    pick = lambda p: pl.BlockSpec((1, rows, dk), lambda h, s: (p, s, h))
    updated, normed = pl.pallas_call(
        state_kernel,
        grid=(heads, local // rows),
        out_shape=(
            jax.ShapeDtypeStruct(state.shape, F32),
            jax.ShapeDtypeStruct((local, heads * dv), F32),
        ),
        in_specs=[
            pick(0), pick(1), pick(2), pick(3),
            pl.BlockSpec((1, dk), lambda h, s: (0, h)),
            pl.BlockSpec((1, dv), lambda h, s: (0, 0)),
            pl.BlockSpec((rows, 1, dk, dv), lambda h, s: (s, h, 0, 0)),
        ],
        out_specs=(
            pl.BlockSpec((rows, 1, dk, dv), lambda h, s: (s, h, 0, 0)),
            pl.BlockSpec((rows, dv), lambda h, s: (s, h)),
        ),
        scratch_shapes=[pltpu.VMEM((rows, dv), F32)],
        name="state",
    )(raw, raw, raw, raw, lower_bound.reshape(1, hid), head_gain.reshape(1, dv), state)

    layer_out = pl.pallas_call(
        functools.partial(mix_kernel, n_kv, n_tp, features),
        out_shape=jax.ShapeDtypeStruct((seqs, width), BF16),
        in_specs=[in_vmem()] * 3 + [in_hbm()] * 4,
        out_specs=in_vmem(),
        scratch_shapes=[
            pltpu.VMEM(w_mix_out.shape, BF16),
            pltpu.VMEM((2, units, depth), BF16),
            pltpu.VMEM(w_down.shape, BF16),
            pltpu.VMEM((local, hid), BF16),
            pltpu.VMEM((seqs, hid), BF16),
            pltpu.VMEM((2, half, seqs, width), BF16),
            pltpu.VMEM((half, seqs, width), BF16),
            pltpu.VMEM((half - 1, seqs, width), BF16),
            pltpu.VMEM((half - 1, seqs, width), BF16),
            pltpu.VMEM((seqs, width), BF16),
            pltpu.VMEM((n_tp, seqs, width), BF16),
            pltpu.VMEM((seqs, depth), BF16),
            pltpu.VMEM((seqs, LANES), F32),
            pltpu.VMEM((n_kv - 1, local, LANES), F32),
            pltpu.VMEM((2, seqs, units), BF16),
            pltpu.VMEM((n_kv - 1, 2, local, units), BF16),
            pltpu.VMEM((local, units), BF16),
            pltpu.VMEM((seqs, units), BF16),
            pltpu.VMEM((2, half, seqs, width), BF16),
            pltpu.VMEM((half, seqs, width), BF16),
            pltpu.VMEM((half - 1, seqs, width), BF16),
            pltpu.VMEM((half - 1, seqs, width), BF16),
            dma((4,)),
            dma((n_kv - 1,)), dma((n_kv - 1,)),
            dma((n_tp - 1,)), dma((n_tp - 1,)),
            dma((n_tp - 1,)), dma((n_tp - 1,)),
            dma((n_kv - 1,)), dma((n_kv - 1,)),
            dma((n_kv - 1, 2)), dma((n_kv - 1, 2)),
            dma((n_kv - 1,)), dma((n_kv - 1,)),
            dma((n_tp - 1,)), dma((n_tp - 1,)),
        ],
        compiler_params=pltpu.CompilerParams(collective_id=1, has_side_effects=True),
        name="mix",
    )(normed, residual, ffn_gain.reshape(1, depth), w_mix_out, w_gate.T, w_up.T, w_down)
    return layer_out, updated


def solution(mesh):
    in_specs = (
        P(None, ("kv", "tp")),
        P("kv"),
        P("kv", "tp"),
        P("kv", "tp"),
        P("kv", "tp"),
        P("kv", "tp"),
        P("tp"),
        P("kv", "tp", None, None),
        P(),
        P("tp", "kv"),
        P("kv"),
        P("kv", "tp"),
        P("kv", "tp"),
        P("tp", "kv"),
    )
    out_specs = (P(None, ("kv", "tp")), P("kv", "tp", None, None))
    return jax.shard_map(
        functools.partial(body, mesh.shape["kv"], mesh.shape["tp"]),
        mesh=mesh, in_specs=in_specs, out_specs=out_specs, check_vma=False,
    )
```
